32 devices in a mesh: grp: 2 (over y), sp: 4 (over z), tp: 4 (over x, core).
Axes of the slice: x: 2, y: 2, z: 4, core: 2. Of those that a mesh axis runs over, the one named last changes fastest.
Arguments:
- tokens: bfloat16 [4096, 2, 2048], P(('grp', 'sp', 'tp')), parts along dimension 0, may hold values from -64 to 64
- w_query: bfloat16 [2048, 2048], P(None, 'tp'), may hold values from -0.21875 to 0.21875
- w_key: bfloat16 [2048, 2048], P(None, 'tp'), may hold values from -0.125 to 0.125
- w_value: bfloat16 [2048, 2048], P(None, 'tp'), may hold values from -0.125 to 0.125
- w_out: bfloat16 [2048, 2048], P('tp'), may hold values from -0.125 to 0.125
- head_lambda: float32 [16], P('tp'), may hold values from 0.3 to 0.8
- sub_gain: float32 [128], replicated, may hold values from 0.1 to 1.9
Outputs:
- mixed: bfloat16 [4096, 2, 2048], P(('grp', 'sp', 'tp')), parts along dimension 0
The draws below stay inside these ranges and needn't reach their ends.
There are 2 independent parts, one for each index of `grp`. The reference program is written for one: setup_inputs(seed, part) draws one part's arguments, and reference() takes and returns one part's arrays. A program takes and returns all parts, laid end to end along the dimension named above; an argument that names none is the same for every part. Nothing has to cross between parts.
All inputs are finite; a program needn't handle non-finite values.
Results may differ from the reference program's by a relative error of at most 0.015.
The reference program's roundings to bfloat16 on the way count: a program that leaves them out, or rounds other values in their place, can miss the bound.
Values may be sent and summed in bfloat16 or wider, within the bound.
No kernel may reach another device: no remote copies, remote signals or barrier semaphores. Data moves between devices by JAX's collectives and lax.ppermute only.
A program may use at most 128 MiB of HBM per device.

```python
import math
import jax
import jax.numpy as jnp
from jax import lax

D = 2048
HEAD = 64
SPAN = 64
SEQS = 2
TOK_DEV = 512
HEADS = 16
LENGTH = 2048
N_TP = 4


def draw_tokens(key, part):
    key_base, key_shift = jax.random.split(jax.random.fold_in(key, 11), 2)
    base = jax.random.normal(key_base, (LENGTH, SEQS, D), jnp.float32)
    shifts = 0.6 * jax.random.normal(key_shift, (LENGTH // TOK_DEV, SEQS, D), jnp.float32)
    base = base + jnp.repeat(shifts, TOK_DEV, axis=0)
    return jnp.clip(base, -64.0, 64.0).astype(jnp.bfloat16)


def steps_of(own_key, dims, cuts, smallest, high):
    loudness, own = 1.0, jax.random.fold_in(own_key, 6)
    for position, blocks in cuts:
        heights = jnp.exp(jax.random.uniform(jax.random.fold_in(own, position), (blocks,), jnp.float32, smallest / len(cuts), high / len(cuts)))
        loudness = loudness * jnp.repeat(heights, dims[position] // blocks).reshape([-1 if axis == position else 1 for axis in range(len(dims))])
    return loudness


def bell_draw(own_key, extent, spread, bound, shards=(), held_as=jnp.bfloat16):
    result = spread * jax.random.normal(own_key, extent, jnp.float32)
    if shards:
        result = result * steps_of(own_key, extent, shards, -0.22, 0.18)
    return jnp.clip(result, -bound, bound).astype(held_as)


def setup_inputs(seed: int = 0, part: int = 0) -> dict:
    keys = jax.random.split(jax.random.key(seed), 8)
    part_splits = jax.random.split(jax.random.fold_in(keys[7], part), 8)
    return {
        "tokens": draw_tokens(jax.random.fold_in(jax.random.fold_in(keys[7], part), 71), part),
        "w_query": bell_draw(keys[1], (D, D), (D // 3) ** -0.5, 0.21875, ((1, 4),)),
        "w_key": bell_draw(keys[2], (D, D), D ** -0.5, 0.125, ((1, 4),)),
        "w_value": bell_draw(keys[3], (D, D), D ** -0.5, 0.125, ((1, 4),)),
        "w_out": bell_draw(keys[4], (D, D), D ** -0.5, 0.125, ((0, 4),)),
        "head_lambda": jnp.clip(0.3 + 0.5 * jax.random.uniform(keys[5], (HEADS,), jnp.float32) ** steps_of(keys[5], (HEADS,), ((0, 4),), -0.2, 0.2), 0.3, 0.8),
        "sub_gain": jnp.clip(1.0 + 0.18 * jax.random.normal(keys[6], (2 * HEAD,), jnp.float32), 0.1, 1.9),
    }


def one_sequence(seq_tokens, w_query, w_key, w_value, w_out, head_lambda, sub_gain):
    total_rows = seq_tokens.shape[0]
    head_count = head_lambda.shape[0]
    value_dim = 2 * HEAD
    queries = jnp.dot(seq_tokens, w_query, preferred_element_type=jnp.float32).astype(jnp.bfloat16)
    queries = queries.reshape(total_rows, head_count, 2, HEAD).transpose(1, 0, 2, 3)
    keys_all = jnp.dot(seq_tokens, w_key, preferred_element_type=jnp.float32).astype(jnp.bfloat16)
    keys_all = keys_all.reshape(total_rows, head_count, 2, HEAD).transpose(1, 0, 2, 3)
    values = jnp.dot(seq_tokens, w_value, preferred_element_type=jnp.float32).astype(jnp.bfloat16)
    values = values.reshape(total_rows, head_count, value_dim).transpose(1, 0, 2)
    blk_len = math.gcd(total_rows, 512)
    blk_count = total_rows // blk_len
    positions = jnp.arange(total_rows, dtype=jnp.int32)

    def one_head(head_args):
        head_q, head_k, head_v, head_lam = head_args
        key_f = head_k.astype(jnp.float32)
        value_f = head_v.astype(jnp.float32)

        def one_block(blk_args):
            query_blk, blk_index = blk_args
            query_pos = blk_index * blk_len + jnp.arange(blk_len, dtype=jnp.int32)
            scores = jnp.einsum('qmd,kmd->mqk', query_blk.astype(jnp.float32), key_f) * HEAD ** (-0.5)
            allowed = (positions // SPAN)[None, :] <= (query_pos // SPAN)[:, None]
            top_val = lax.optimization_barrier(jnp.max(jnp.where(allowed, scores, -jnp.inf), axis=-1, keepdims=True))
            expo_vals = jnp.where(allowed, jnp.exp(scores - top_val), 0.0)
            sums = lax.optimization_barrier(jnp.sum(expo_vals, axis=-1))
            rounded = lax.optimization_barrier(expo_vals.astype(jnp.bfloat16)).astype(jnp.float32)
            accum = jnp.einsum('mqk,ke->mqe', rounded, value_f)
            return accum[0] / sums[0][:, None] - head_lam * accum[1] / sums[1][:, None]
        blocks_out = lax.map(one_block, (head_q.reshape(blk_count, blk_len, 2, HEAD), jnp.arange(blk_count, dtype=jnp.int32)))
        return blocks_out.reshape(total_rows, value_dim)
    attn = lax.map(one_head, (queries, keys_all, values, head_lambda))
    mean_sq = lax.optimization_barrier(jnp.mean(attn * attn, axis=-1, keepdims=True))
    normed = (attn * lax.rsqrt(mean_sq + 1e-06) * sub_gain).astype(jnp.bfloat16)
    normed = normed.transpose(1, 0, 2).reshape(total_rows, head_count * value_dim)
    group_cols = head_count * value_dim // N_TP
    summed = jnp.zeros((total_rows, w_out.shape[1]), jnp.float32)
    for group in range(N_TP):
        partial_out = jnp.dot(normed[:, group * group_cols:(group + 1) * group_cols], w_out[group * group_cols:(group + 1) * group_cols], preferred_element_type=jnp.float32)
        summed = summed + lax.optimization_barrier(partial_out.astype(jnp.bfloat16)).astype(jnp.float32)
    return summed.astype(jnp.bfloat16)

def reference(tokens, w_query, w_key, w_value, w_out, head_lambda, sub_gain):
    outputs = []
    for seq_index in range(tokens.shape[1]):
        outputs.append(one_sequence(tokens[:, seq_index], w_query, w_key, w_value, w_out, head_lambda, sub_gain))
    return jnp.stack(outputs, axis=1)
```

```python
import functools
import math

import jax
import jax.numpy as jnp
from jax import lax
from jax.experimental import pallas as pl
from jax.experimental.pallas import tpu as pltpu
from jax.sharding import PartitionSpec as P

SPAN = 64


NEG_FILL = -1e30
EPS_NORM = 1e-06
VMEM_LIMIT = 60 * 1024 * 1024


def key_block(state_in, queries, query_pos, key_blk, value_blk, key_start):
    run_max, run_sum, run_acc = state_in
    blk_len = key_blk.shape[0]
    heads_here = queries.shape[1]
    head_dim = queries.shape[3]
    key_pos = key_start + jnp.arange(blk_len, dtype=jnp.int32)
    key_four = key_blk.reshape(blk_len, heads_here, 2, head_dim)
    scores = jnp.einsum("qhmd,khmd->mhqk", queries, key_four, preferred_element_type=jnp.float32)
    scores = scores * head_dim ** (-0.5)
    allowed = (key_pos // SPAN)[None, :] <= (query_pos // SPAN)[:, None]
    new_max = jnp.maximum(run_max, jnp.max(jnp.where(allowed, scores, NEG_FILL), axis=-1))
    expo_vals = jnp.where(allowed, jnp.exp(scores - new_max[..., None]), 0.0)
    factor = jnp.exp(run_max - new_max)
    run_sum = run_sum * factor + jnp.sum(expo_vals, axis=-1)
    value_three = value_blk.reshape(blk_len, heads_here, 2 * head_dim)
    mixed_vals = jnp.einsum(
        "mhqk,khe->mhqe",
        expo_vals.astype(jnp.bfloat16),
        value_three,
        preferred_element_type=jnp.float32,
    )
    run_acc = run_acc * factor[..., None] + mixed_vals
    return (new_max, run_sum, run_acc)


def guarded_block(state_in, queries, query_pos, key_blk, value_blk, key_start):
    last_pos = query_pos[-1]

    def compute(inner_state):
        return key_block(inner_state, queries, query_pos, key_blk, value_blk, key_start)

    def keep(inner_state):
        return inner_state

    return lax.cond(key_start <= last_pos, compute, keep, state_in)


def sequence_piece(state_in, queries, query_pos, key_part, value_part):
    length = key_part.shape[0]
    step_len = math.gcd(length, 512)
    step_count = length // step_len

    def one_step(step_index, inner_state):
        offset = step_index * step_len
        key_blk = lax.dynamic_slice_in_dim(key_part, offset, step_len, 0)
        value_blk = lax.dynamic_slice_in_dim(value_part, offset, step_len, 0)
        return guarded_block(inner_state, queries, query_pos, key_blk, value_blk, offset)

    return lax.fori_loop(0, step_count, one_step, state_in)


def normalize(attn, sub_gain):
    mean_sq = jnp.mean(attn * attn, axis=-1, keepdims=True)
    normed = (attn * lax.rsqrt(mean_sq + EPS_NORM) * sub_gain).astype(jnp.bfloat16)
    return jnp.transpose(normed, (1, 0, 2)).reshape(attn.shape[1], attn.shape[0] * attn.shape[2])


def gathered_plan(tokens, w_query, w_key, w_value, w_out, head_lambda, sub_gain):
    tp_count = lax.axis_size("tp")
    tok_rows = tokens.shape[0] * tp_count
    seq_count = tokens.shape[1]
    heads_here = head_lambda.shape[0]
    head_dim = w_query.shape[1] // (2 * heads_here)
    value_dim = 2 * head_dim
    query_cols = w_query.shape[1]
    w_joined = jnp.concatenate([w_query, w_key, w_value], axis=1)
    joined = jnp.dot(
        lax.all_gather(tokens, "tp", axis=0, tiled=True),
        w_joined,
        preferred_element_type=jnp.float32,
    ).astype(jnp.bfloat16)
    query_flat = joined[:, :, :query_cols]
    keys_here = joined[:, :, query_cols : 2 * query_cols]
    values_here = joined[:, :, 2 * query_cols :]
    sp_index = lax.axis_index("sp")
    own_first = sp_index * tok_rows
    lam_col = head_lambda[:, None, None]

    def attend(query_sets, first_rows):
        positions = [first + jnp.arange(tok_rows, dtype=jnp.int32) for first in first_rows]
        query_four = [qset.reshape(tok_rows, heads_here, 2, head_dim) for qset in query_sets]
        start_one = (
            jnp.full((2, heads_here, tok_rows), NEG_FILL, jnp.float32),
            jnp.zeros((2, heads_here, tok_rows), jnp.float32),
            jnp.zeros((2, heads_here, tok_rows, value_dim), jnp.float32),
        )
        start_state = tuple((start_one for seq_index in range(seq_count)))
        key_part = lax.all_gather(keys_here, "sp", axis=0, tiled=True)
        value_part = lax.all_gather(values_here, "sp", axis=0, tiled=True)
        new_states = []
        for seq_index in range(seq_count):
            new_states.append(
                sequence_piece(
                    start_state[seq_index],
                    query_four[seq_index],
                    positions[seq_index],
                    key_part[:, seq_index],
                    value_part[:, seq_index],
                )
            )
        final_states = tuple(new_states)
        results = []
        for run_max, run_sum, run_acc in final_states:
            attn = run_acc[0] / run_sum[0][..., None] - lam_col * run_acc[1] / run_sum[1][..., None]
            results.append(normalize(attn, sub_gain))
        return results

    normed_list = attend(
        [query_flat[:, seq_index] for seq_index in range(seq_count)],
        [own_first for seq_index in range(seq_count)],
    )
    normed = jnp.stack(normed_list, axis=1)
    return lax.psum_scatter(
        jnp.dot(normed, w_out, preferred_element_type=jnp.float32).astype(jnp.bfloat16),
        "tp",
        scatter_dimension=0,
        tiled=True,
    )


ANY = pl.BlockSpec(memory_space=pl.ANY)
VMEM = pl.BlockSpec(memory_space=pltpu.VMEM)
SMEM = pl.BlockSpec(memory_space=pltpu.SMEM)


def project_kernel(pieces, ids, *refs):
    piece_refs = refs[:pieces]
    w_query, w_key, w_value, out_ref, rows_buf, sems = refs[pieces:]
    piece_rows = piece_refs[0].shape[0]
    cols = out_ref.shape[1] // 3
    me = ids[1]
    copies = []
    for index in range(pieces):
        start = pl.multiple_of((me ^ index) * piece_rows, piece_rows)
        copies.append(
            pltpu.make_async_copy(piece_refs[index], rows_buf.at[pl.ds(start, piece_rows)], sems.at[index])
        )
    for copy in copies:
        copy.start()
    for copy in copies:
        copy.wait()
    for index, w_ref in enumerate((w_query, w_key, w_value)):
        out_ref[:, index * cols : (index + 1) * cols] = jnp.dot(
            rows_buf[...], w_ref[...], preferred_element_type=jnp.float32
        ).astype(jnp.bfloat16)


def project(ids, pieces, w_query, w_key, w_value, cols):
    count = len(pieces)
    piece_rows, depth = pieces[0].shape
    rows = count * piece_rows
    w_spec = pl.BlockSpec((depth, cols), lambda step, ids: (0, ids[0]))
    return pl.pallas_call(
        functools.partial(project_kernel, count),
        grid_spec=pltpu.PrefetchScalarGridSpec(
            num_scalar_prefetch=1,
            grid=(1,),
            in_specs=[ANY] * count + [w_spec] * 3,
            out_specs=pl.BlockSpec((rows, 3 * cols), lambda step, ids: (0, 0)),
            scratch_shapes=[
                pltpu.VMEM((rows, depth), jnp.bfloat16),
                pltpu.SemaphoreType.DMA((count,)),
            ],
        ),
        out_shape=jax.ShapeDtypeStruct((rows, 3 * cols), jnp.bfloat16),
        compiler_params=pltpu.CompilerParams(vmem_limit_bytes=VMEM_LIMIT),
        cost_estimate=pl.CostEstimate(
            flops=2 * rows * depth * 3 * cols,
            bytes_accessed=2 * (rows * depth + 3 * depth * cols + 3 * rows * cols),
            transcendentals=0,
        ),
        name="project",
    )(ids, *pieces, w_query, w_key, w_value)


def attend_kernel(shards, parts, tile, ids, *refs):
    chunk_refs = refs[:shards]
    lam_ref, gain_ref = refs[shards : shards + 2]
    outs = refs[shards + 2 : shards + 2 + shards * parts // 2]
    qkv_buf, score_buf, out_buf, sems, out_sems = refs[shards + 2 + shards * parts // 2 :]
    rows = chunk_refs[0].shape[0]
    length = qkv_buf.shape[0]
    cols = qkv_buf.shape[1] // 3
    value_dim = gain_ref.shape[1]
    heads = cols // value_dim
    head_dim = value_dim // 2
    piece_rows = rows // parts
    z_here, t_here = ids[2], ids[1]
    copies = []
    for index in range(shards):
        start = pl.multiple_of((z_here ^ index) * rows, rows)
        copies.append(
            pltpu.make_async_copy(chunk_refs[index], qkv_buf.at[pl.ds(start, rows)], sems.at[index])
        )
    for copy in copies:
        copy.start()
    for copy in copies:
        copy.wait()

    lanes = lax.broadcasted_iota(jnp.int32, (tile, value_dim), 1)
    first_map = lanes < head_dim
    ones = jnp.ones((tile, value_dim), jnp.bfloat16)
    span_q = lax.broadcasted_iota(jnp.int32, (2 * tile, tile), 0) % tile // SPAN
    span_k = lax.broadcasted_iota(jnp.int32, (2 * tile, tile), 1) // SPAN
    allowed = span_k <= span_q
    scale = head_dim ** (-0.5)

    @pl.loop(0, heads)
    def one_head(head):
        def lane_slab(base):
            return pl.ds(pl.multiple_of(base + head * value_dim, value_dim), value_dim)

        lam = lam_ref[head]
        for q_tile in range(length // tile):
            q_rows = pl.ds(q_tile * tile, tile)
            query = qkv_buf[q_rows, lane_slab(0)] * jnp.bfloat16(scale)
            zero = jnp.zeros_like(query)
            both = jnp.concatenate(
                [jnp.where(first_map, query, zero), jnp.where(first_map, zero, query)], axis=0
            )
            top = None
            for k_tile in range(q_tile + 1):
                key = qkv_buf[pl.ds(k_tile * tile, tile), lane_slab(cols)]
                scores = lax.dot_general(
                    both, key, (((1,), (1,)), ((), ())), preferred_element_type=jnp.float32
                )
                if k_tile == q_tile:
                    scores = jnp.where(allowed, scores, NEG_FILL)
                score_buf[:, k_tile * tile : (k_tile + 1) * tile] = scores
                tile_top = functools.reduce(
                    jnp.maximum,
                    [scores[:, c : c + 128] for c in range(0, tile, 128)],
                )
                top = tile_top if top is None else jnp.maximum(top, tile_top)
            top = jnp.max(top, axis=1, keepdims=True)
            acc = None
            for k_tile in range(q_tile + 1):
                scores = score_buf[:, k_tile * tile : (k_tile + 1) * tile]
                expo = jnp.exp(scores - top).astype(jnp.bfloat16)
                value = qkv_buf[pl.ds(k_tile * tile, tile), lane_slab(2 * cols)]
                term = jnp.dot(
                    expo, jnp.concatenate([value, ones], axis=1), preferred_element_type=jnp.float32
                )
                acc = term if acc is None else acc + term
            ratio = acc[:, :value_dim] / acc[:, value_dim:]
            attn = ratio[:tile] - lam * ratio[tile:]
            mean_sq = jnp.mean(attn * attn, axis=1, keepdims=True)
            normed = (attn * lax.rsqrt(mean_sq + EPS_NORM) * gain_ref[...]).astype(jnp.bfloat16)
            for piece in range(tile // piece_rows):
                block = q_tile * (tile // piece_rows) + piece
                shard, part = block // parts, block % parts
                other = part ^ t_here
                out_buf[
                    z_here ^ shard,
                    other & 1,
                    other >> 1,
                    :,
                    lane_slab(0),
                ] = normed[piece * piece_rows : (piece + 1) * piece_rows]

    out_copies = []
    for index, out_ref in enumerate(outs):
        out_copies.append(
            pltpu.make_async_copy(out_buf.at[index // 2, index % 2], out_ref, out_sems.at[index])
        )
    for copy in out_copies:
        copy.start()
    for copy in out_copies:
        copy.wait()


def attend(ids, chunks, lam_here, gain, parts):
    shards = len(chunks)
    rows, all_cols = chunks[0].shape
    length = shards * rows
    cols = all_cols // 3
    value_dim = gain.shape[1]
    heads = cols // value_dim
    piece_rows = rows // parts
    tile = 2 * piece_rows
    n_out = shards * parts // 2
    out_shape = jax.ShapeDtypeStruct((2, piece_rows, cols), jnp.bfloat16)
    scored = heads * 2 * length * (length + tile) // 2
    return pl.pallas_call(
        functools.partial(attend_kernel, shards, parts, tile),
        in_specs=[SMEM] + [ANY] * shards + [SMEM, VMEM],
        out_specs=[ANY] * n_out,
        out_shape=[out_shape] * n_out,
        scratch_shapes=[
            pltpu.VMEM((length, all_cols), jnp.bfloat16),
            pltpu.VMEM((2 * tile, length), jnp.float32),
            pltpu.VMEM((shards, 2, parts // 2, piece_rows, cols), jnp.bfloat16),
            pltpu.SemaphoreType.DMA((shards,)),
            pltpu.SemaphoreType.DMA((n_out,)),
        ],
        compiler_params=pltpu.CompilerParams(vmem_limit_bytes=VMEM_LIMIT),
        cost_estimate=pl.CostEstimate(
            flops=2 * scored * 4 * value_dim,
            bytes_accessed=2 * length * (all_cols + cols),
            transcendentals=scored,
        ),
        name="attend",
    )(ids, *chunks, lam_here, gain)


def mix_kernel(shards, side, ids, *refs):
    n_in = 2 * shards
    w_own, w_near, out_ref, rows_buf, sems = refs[n_in:]
    in_refs = refs[:n_in]
    piece_rows, cols = in_refs[0].shape[1:]
    z_here = ids[2]
    half, low = z_here // 2, z_here % 2

    @pl.when(pl.program_id(0) == 0)
    def load_rows():
        copies = []
        for index, in_ref in enumerate(in_refs):
            z_xor, t_xor = index // 2, index % 2
            seq = half ^ (z_xor // 2)
            row = pl.multiple_of(seq * piece_rows, piece_rows)
            lane = pl.multiple_of((low ^ (z_xor % 2)) * cols + 2 * t_xor * cols, cols)
            copies.append(
                pltpu.make_async_copy(
                    in_ref.at[side],
                    rows_buf.at[pl.ds(row, piece_rows), pl.ds(lane, cols)],
                    sems.at[index],
                )
            )
        for copy in copies:
            copy.start()
        for copy in copies:
            copy.wait()

    own_depth = w_own.shape[0]
    out_ref[...] = (
        jnp.dot(rows_buf[:, :own_depth], w_own[...], preferred_element_type=jnp.float32)
        + jnp.dot(rows_buf[:, own_depth:], w_near[...], preferred_element_type=jnp.float32)
    ).astype(out_ref.dtype)


def mix(ids, parts_in, w_own, w_near, side, out_dtype):
    shards = len(parts_in) // 2
    piece_rows, cols = parts_in[0].shape[1:]
    depth, width = w_own.shape
    rows = 2 * piece_rows
    block = min(width, 512)
    return pl.pallas_call(
        functools.partial(mix_kernel, shards, side),
        grid_spec=pltpu.PrefetchScalarGridSpec(
            num_scalar_prefetch=1,
            grid=(width // block,),
            in_specs=[ANY] * len(parts_in)
            + [pl.BlockSpec((depth, block), lambda step, ids: (0, step))] * 2,
            out_specs=pl.BlockSpec((rows, block), lambda step, ids: (0, step)),
            scratch_shapes=[
                pltpu.VMEM((rows, 2 * depth), jnp.bfloat16),
                pltpu.SemaphoreType.DMA((len(parts_in),)),
            ],
        ),
        out_shape=jax.ShapeDtypeStruct((rows, width), out_dtype),
        compiler_params=pltpu.CompilerParams(vmem_limit_bytes=VMEM_LIMIT),
        cost_estimate=pl.CostEstimate(
            flops=4 * rows * depth * width,
            bytes_accessed=2 * (2 * rows * depth + 2 * depth * width + rows * width),
            transcendentals=0,
        ),
        name=f"mix_{side}",
    )(ids, *parts_in, w_own, w_near)


def swap(value, axis, distance):
    size = lax.axis_size(axis)
    return lax.ppermute(value, axis, [(index, index ^ distance) for index in range(size)])


def swap_both(value, z_xor, t_xor):
    sp, tp = lax.axis_size("sp"), lax.axis_size("tp")
    pairs = [
        (z * tp + t, (z ^ z_xor) * tp + (t ^ t_xor)) for z in range(sp) for t in range(tp)
    ]
    return lax.ppermute(value, ("sp", "tp"), pairs)


def split_plan(tokens, w_query, w_key, w_value, w_out, head_lambda, sub_gain):
    z_here = lax.axis_index("sp")
    t_here = lax.axis_index("tp")
    tp = lax.axis_size("tp")
    half, low = z_here // 2, z_here % 2
    heads_mine = head_lambda.shape[0] // 2
    cols = w_query.shape[1] // 2
    ids = jnp.stack([low, t_here, z_here]).astype(jnp.int32)
    own = lax.dynamic_index_in_dim(tokens, half, 1, keepdims=False)
    away = lax.dynamic_index_in_dim(tokens, 1 - half, 1, keepdims=False)
    far = swap(away, "sp", 2)
    near = swap(own, "sp", 1)
    far_near = swap(far, "sp", 1)
    w_near = swap(w_out, "tp", 1)
    chunks = []
    for piece in (own, near, far, far_near):
        crossed = swap(piece, "tp", 2)
        pieces = [piece, swap(piece, "tp", 1), crossed, swap(crossed, "tp", 1)]
        chunks.append(project(ids, pieces, w_query, w_key, w_value, cols))
    lam_here = lax.dynamic_slice_in_dim(head_lambda, low * heads_mine, heads_mine, 0)
    outs = attend(ids, chunks, lam_here, sub_gain[None, :], tp)
    received = [outs[0]]
    for index in range(1, len(outs)):
        received.append(swap_both(outs[index], index // 2, index % 2))
    partial = swap(mix(ids, received, w_out, w_near, 1, jnp.bfloat16), "tp", 2)
    kept = mix(ids, received, w_out, w_near, 0, jnp.float32)
    total = (kept + partial.astype(jnp.float32)).astype(jnp.bfloat16)
    return jnp.transpose(total.reshape(2, tokens.shape[0], total.shape[1]), (1, 0, 2))


def on_device(tokens, w_query, w_key, w_value, w_out, head_lambda, sub_gain):
    seqs = tokens.shape[1]
    sp, tp = lax.axis_size("sp"), lax.axis_size("tp")
    heads_here = head_lambda.shape[0]
    lane_heads = w_query.shape[1] // heads_here % 128 == 0
    whole_tiles = tokens.shape[0] % 128 == 0
    if seqs == 2 and sp == 4 and tp == 4 and heads_here % 2 == 0 and lane_heads and whole_tiles:
        plan = split_plan
    else:
        plan = gathered_plan
    return plan(tokens, w_query, w_key, w_value, w_out, head_lambda, sub_gain)


def solution(mesh):
    return jax.shard_map(
        on_device,
        mesh=mesh,
        in_specs=(
            P(("grp", "sp", "tp"), None, None),
            P(None, "tp"),
            P(None, "tp"),
            P(None, "tp"),
            P("tp", None),
            P("tp"),
            P(),
        ),
        out_specs=P(("grp", "sp", "tp"), None, None),
        check_vma=False,
    )
```
